32 devices in a mesh: ep: 8 (over z, x), tp: 4 (over y, core).
Axes of the slice: x: 2, y: 2, z: 4, core: 2. Of those that a mesh axis runs over, the one named last changes fastest.
Arguments:
- x_attend: bfloat16 [4096, 2048], P('ep'), may hold values from -6 to 6
- attend_gain: float32 [2048], replicated, may hold values from 0.1 to 1.9
- w_query: bfloat16 [2048, 1024], P(None, 'tp'), may hold values from -0.125 to 0.125
- w_key: bfloat16 [2048, 512], P(None, 'tp'), may hold values from -0.125 to 0.125
- w_value: bfloat16 [2048, 512], P(None, 'tp'), may hold values from -0.125 to 0.125
- query_gain: float32 [64], replicated, may hold values from 0.1 to 1.9
- key_gain: float32 [64], replicated, may hold values from 0.1 to 1.9
- sink_logit: float32 [16], P('tp'), may hold values from 4 to 8
- w_output: bfloat16 [1024, 2048], P('tp'), may hold values from -1.5 to 1.5
- x_experts: bfloat16 [3072, 2048], P('ep'), may hold values from -6 to 6
- expert_gain: float32 [2048], replicated, may hold values from 0.1 to 1.9
- routes: int32 [3072, 2], P('ep'), may hold values from 0 to 7, all different within a row; in each aligned block of 384 rows (0 to 383, 384 to 767, ...) at most 144 rows name the same one
- group_prob: float32 [3072], P('ep'), may hold values from 0.3 to 1
- expert_prob: float32 [3072, 2], P('ep'), may hold values from 0.05 to 1
- w_gate: bfloat16 [8, 2048, 1024], P('ep', None, 'tp'), may hold values from -0.125 to 0.125
- w_up: bfloat16 [8, 2048, 1024], P('ep', None, 'tp'), may hold values from -0.125 to 0.125
- w_down: bfloat16 [8, 1024, 2048], P('ep', 'tp'), may hold values from -0.1875 to 0.1875
Outputs:
- attend_out: bfloat16 [4096, 2048], P(('ep', 'tp'))
- expert_out: bfloat16 [3072, 2048], P('ep', 'tp')
The draws below stay inside these ranges and needn't reach their ends.
Inputs may be any that keep to these rules, and one draw needn't show every extreme that they name: `routes`: each row names 2 different experts. Among the rows of one device no expert is named more than 144 times, and in every draw some expert is named exactly 144 times by one device's rows.
All inputs are finite; a program needn't handle non-finite values.
Results may differ from the reference program's by a relative error of at most 0.012.
Values may be sent and summed in bfloat16 or wider, within the bound.
A program may use at most 64 MiB of HBM per device.

```python
import math
import jax
import jax.numpy as jnp
import numpy as np
from jax import lax

D = 2048
HEADS = 16
KV_HEADS = 8
HEAD_DIM = 64
FF = 1024
TOPK = 2
WINDOW = 128
GRID_W = 64
TOK_A = 512
TOK_M = 384
EXPERTS = 8
CAP = 144
TOKENS_A = 4096
TOKENS_M = 3072
N_EP = 8
N_TP = 4


def levels(rng, shape, pieces, smallest, high):
    factor_of = 1.0
    for dim, blocks in pieces:
        heights = jax.random.uniform(jax.random.fold_in(jax.random.fold_in(rng, 6), dim), (blocks,), jnp.float32, smallest / len(pieces), high / len(pieces))
        factor_of = factor_of * jnp.repeat(jnp.exp(heights), shape[dim] // blocks).reshape((-1,) + (1,) * (len(shape) - 1 - dim))
    return factor_of


def assign_block(rng, own, number, rows, amount, top, reach, slope):
    ranking = jax.random.permutation(rng, amount)
    heavy_load, ordinary = shares(amount, rows * top, reach, slope, True), shares(amount, rows * top, reach, slope, False)
    places = jnp.arange(amount)

    def named(tallies, offset_by):
        used = int((tallies > 0).sum())
        fixed = max(1, used // 4)
        moved = fixed + (places - fixed + offset_by * (used - fixed)) % max(1, amount - fixed)
        return jnp.zeros((amount,), jnp.int32).at[ranking[jnp.where(places < fixed, places, moved)]].set(jnp.asarray(tallies, jnp.int32))

    tallies = jnp.where(number % 4 == 0, named(heavy_load, number // 4), named(ordinary, number - number // 4 - 1))
    mixed = jax.random.permutation(jax.random.fold_in(own, 3), amount)
    giver, sink = mixed[0:amount // 2 * 2:2], mixed[1:amount // 2 * 2:2]
    slack = jnp.minimum(tallies[giver] - 1, reach - tallies[sink]) // 2
    slack = jnp.where((giver == ranking[0]) | (sink == ranking[0]) | (tallies[sink] == 0), 0, jnp.maximum(slack, 0))
    moved = jax.random.randint(jax.random.fold_in(own, 4), (amount // 2,), 0, 1 << 20) % (slack + 1)
    tallies = tallies.at[giver].add(-moved).at[sink].add(moved)
    labels = jnp.searchsorted(jnp.cumsum(tallies), jnp.arange(rows * top), side="right").astype(jnp.int32)
    listing = labels.reshape(top, rows).T
    listing = listing[jax.random.permutation(jax.random.fold_in(own, 1), rows)]
    offset_by = jax.random.randint(jax.random.fold_in(own, 2), (rows, 1), 0, top)
    return jnp.take_along_axis(listing, (jnp.arange(top)[None, :] + offset_by) % top, axis=1)


def shares(amount, total, reach, skew, full):
    loads = [(1 << 20) // math.isqrt(grade ** skew) + 1 for grade in range(1, amount + 1)]
    largest = reach if full else min(reach, max(-(-total // amount), total * loads[0] // sum(loads)))
    least = 1 if total - largest >= amount - 1 else 0
    holding, surplus = [largest] + [least] * (amount - 1), total - largest - least * (amount - 1)
    while surplus > 0:
        free = [i for i in range(1, amount) if holding[i] < largest] or [i for i in range(1, amount) if holding[i] < reach]
        whole, remaining = sum([loads[i] for i in free]), surplus
        for i in free:
            extra = min(reach - holding[i], max(1, remaining * loads[i] // whole), surplus)
            holding[i] = holding[i] + extra
            surplus = surplus - extra
    return np.array(holding)


def gaussian(key, dims, width, bound, cuts=(), kind=jnp.bfloat16):
    level = levels(key, dims, cuts, -0.22, 0.18) if cuts else 1.0
    values = jax.random.normal(key, dims, jnp.float32) * width * level
    return jnp.minimum(jnp.maximum(values, -bound), bound).astype(kind)


def setup_inputs(seed: int = 0) -> dict:
    arg_keys = jax.random.split(jax.random.key(seed), 18)
    x_attend = gaussian(arg_keys[0], (TOKENS_A, D), 1.0, 6.0, ((0, 8),))
    attend_gain = jnp.clip(1.0 + 0.18 * jax.random.normal(arg_keys[1], (D,), jnp.float32), 0.1, 1.9)
    w_query = gaussian(arg_keys[2], (D, HEADS * HEAD_DIM), D ** -0.5, 0.125, ((1, 4),))
    w_key = gaussian(arg_keys[3], (D, KV_HEADS * HEAD_DIM), D ** -0.5, 0.125, ((1, 4),))
    w_value = gaussian(arg_keys[4], (D, KV_HEADS * HEAD_DIM), D ** -0.5, 0.125, ((1, 4),))
    query_gain = jnp.clip(1.0 + 0.18 * jax.random.normal(arg_keys[5], (HEAD_DIM,), jnp.float32), 0.1, 1.9)
    key_gain = jnp.clip(1.0 + 0.18 * jax.random.normal(arg_keys[6], (HEAD_DIM,), jnp.float32), 0.1, 1.9)
    sink_logit = jnp.clip(4.0 + 4.0 * jax.random.uniform(arg_keys[7], (HEADS,), jnp.float32) ** levels(arg_keys[7], (HEADS,), ((0, 4),), -0.2, 0.2), 4.0, 8.0)
    w_output = gaussian(arg_keys[8], (HEADS * HEAD_DIM, D), (HEAD_DIM // 4) ** -0.5, 1.5, ((0, 4),))
    x_experts = gaussian(arg_keys[9], (TOKENS_M, D), 1.0, 6.0, ((0, 8),))
    expert_gain = jnp.clip(1.0 + 0.18 * jax.random.normal(arg_keys[10], (D,), jnp.float32), 0.1, 1.9)
    routes_keys = jax.random.split(jax.random.fold_in(arg_keys[11], 1), TOKENS_M // TOK_M)
    routes_turns = jax.random.permutation(jax.random.fold_in(arg_keys[11], 3), TOKENS_M // TOK_M)
    routes = jax.vmap(lambda own, number: assign_block(jax.random.fold_in(arg_keys[11], 2), own, number, TOK_M, EXPERTS, TOPK, CAP, 2))(routes_keys, routes_turns).reshape((TOKENS_M, TOPK))
    group_prob = jnp.clip(0.3 + 0.7 * jax.random.uniform(arg_keys[12], (TOKENS_M,), jnp.float32) ** levels(arg_keys[12], (TOKENS_M,), ((0, 8),), -0.2, 0.2), 0.3, 1.0)
    expert_prob = jnp.clip(0.05 + 0.95 * jax.random.uniform(arg_keys[13], (TOKENS_M, TOPK), jnp.float32) ** levels(arg_keys[13], (TOKENS_M, TOPK), ((0, 8),), -0.2, 0.2), 0.05, 1.0)
    w_gate = gaussian(arg_keys[14], (EXPERTS, D, FF), D ** -0.5, 0.125, ((0, 8), (2, 4)))
    w_up = gaussian(arg_keys[15], (EXPERTS, D, FF), D ** -0.5, 0.125, ((0, 8), (2, 4)))
    w_down = gaussian(arg_keys[16], (EXPERTS, FF, D), FF ** -0.5, 0.1875, ((0, 8), (1, 4)))
    return dict(x_attend=x_attend, attend_gain=attend_gain, w_query=w_query, w_key=w_key, w_value=w_value, query_gain=query_gain, key_gain=key_gain, sink_logit=sink_logit, w_output=w_output, x_experts=x_experts, expert_gain=expert_gain, routes=routes, group_prob=group_prob, expert_prob=expert_prob, w_gate=w_gate, w_up=w_up, w_down=w_down)


epsilon = 1e-06
rope_base = 10000.0

def rms_scale(inputs, gain):
    values_f = inputs.astype(jnp.float32)
    scaled = values_f * lax.rsqrt(lax.optimization_barrier(jnp.mean(values_f * values_f, axis=-1, keepdims=True)) + epsilon)
    return (scaled * gain).astype(jnp.bfloat16)

def rope_tables(positions):
    grid_rows = (positions // GRID_W).astype(jnp.float32)
    grid_cols = (positions % GRID_W).astype(jnp.float32)
    half_dim = HEAD_DIM // 2
    inverse = rope_base ** (-jnp.arange(0, half_dim, 2, dtype=jnp.float32) / half_dim)
    angles = jnp.concatenate([grid_rows[:, None] * inverse, grid_cols[:, None] * inverse], axis=-1)
    return (jnp.cos(angles), jnp.sin(angles))

def head_norm_rope(projected, gain, cosine, sine_tab):
    scaled = projected * lax.rsqrt(lax.optimization_barrier(jnp.mean(projected * projected, axis=-1, keepdims=True)) + epsilon) * gain
    first_half, second_half = jnp.split(scaled, 2, axis=-1)
    cos_b = cosine[:, None, :]
    sin_b = sine_tab[:, None, :]
    turned = jnp.concatenate([first_half * cos_b - second_half * sin_b, second_half * cos_b + first_half * sin_b], axis=-1)
    return turned.astype(jnp.bfloat16)

def slot_plan(route_block):
    flat_ids = route_block.reshape(-1).astype(jnp.int32)
    onehot = (flat_ids[:, None] == jnp.arange(EXPERTS, dtype=jnp.int32)[None, :]).astype(jnp.int32)
    rank_in = jnp.cumsum(onehot, axis=0) - onehot
    slot_pos = lax.optimization_barrier(jnp.sum(rank_in * onehot, axis=1))
    dest_slot = (flat_ids * CAP + slot_pos).astype(jnp.int32)
    owner_tok = (jnp.arange(TOK_M * TOPK, dtype=jnp.int32) // TOPK).astype(jnp.int32)
    slot_tok = jnp.full((EXPERTS * CAP,), TOK_M, jnp.int32).at[dest_slot].set(owner_tok)
    return (dest_slot, slot_tok)

def reference(x_attend, attend_gain, w_query, w_key, w_value, query_gain, key_gain, sink_logit, w_output, x_experts, expert_gain, routes, group_prob, expert_prob, w_gate, w_up, w_down):
    normed = rms_scale(x_attend, attend_gain)
    positions = jnp.arange(TOKENS_A, dtype=jnp.int32)
    cosine, sine_tab = rope_tables(positions)
    queries = head_norm_rope(jnp.dot(normed, w_query, preferred_element_type=jnp.float32).reshape(TOKENS_A, HEADS, HEAD_DIM), query_gain, cosine, sine_tab)
    key_rows = head_norm_rope(jnp.dot(normed, w_key, preferred_element_type=jnp.float32).reshape(TOKENS_A, KV_HEADS, HEAD_DIM), key_gain, cosine, sine_tab)
    values = jnp.dot(normed, w_value, preferred_element_type=jnp.float32).astype(jnp.bfloat16).reshape(TOKENS_A, KV_HEADS, HEAD_DIM)
    key_pad = jnp.pad(key_rows, ((WINDOW, WINDOW), (0, 0), (0, 0)))
    value_pad = jnp.pad(values, ((WINDOW, WINDOW), (0, 0), (0, 0)))
    group = HEADS // KV_HEADS
    sink_col = sink_logit.reshape(KV_HEADS, group)[:, :, None]

    def one_block(blk_idx):
        row_zero = (blk_idx * TOK_A).astype(jnp.int32)
        query_blk = lax.dynamic_slice_in_dim(queries, row_zero, TOK_A, 0).reshape(TOK_A, KV_HEADS, group, HEAD_DIM).astype(jnp.float32)
        key_blk = lax.dynamic_slice_in_dim(key_pad, row_zero, TOK_A + 2 * WINDOW, 0).astype(jnp.float32)
        value_blk = lax.dynamic_slice_in_dim(value_pad, row_zero, TOK_A + 2 * WINDOW, 0).astype(jnp.float32)
        scores = jnp.einsum('qhgd,khd->hgqk', query_blk, key_blk) * HEAD_DIM ** (-0.5)
        query_pos = row_zero + jnp.arange(TOK_A, dtype=jnp.int32)
        key_pos = row_zero - WINDOW + jnp.arange(TOK_A + 2 * WINDOW, dtype=jnp.int32)
        in_window = (jnp.abs(query_pos[:, None] - key_pos[None, :]) <= WINDOW) & (key_pos[None, :] >= 0) & (key_pos[None, :] < TOKENS_A)
        scores = jnp.where(in_window[None, None], scores, -1e+30)
        peak = jnp.maximum(lax.optimization_barrier(jnp.max(scores, axis=-1)), sink_col)[..., None]
        weights = jnp.exp(scores - peak)
        denominator = lax.optimization_barrier(jnp.sum(weights, axis=-1, keepdims=True)) + jnp.exp(sink_col[..., None] - peak)
        probs = (weights / denominator).astype(jnp.bfloat16)
        attended_blk = jnp.einsum('hgqk,khd->qhgd', probs.astype(jnp.float32), value_blk)
        return attended_blk.astype(jnp.bfloat16).reshape(TOK_A, HEADS * HEAD_DIM)
    attended = lax.map(one_block, jnp.arange(N_EP, dtype=jnp.int32)).reshape(TOKENS_A, HEADS * HEAD_DIM)
    head_cols = HEADS * HEAD_DIM // N_TP
    total = jnp.zeros((TOKENS_A, D), jnp.float32)
    for part_idx in range(N_TP):
        partial_value = jnp.dot(attended[:, part_idx * head_cols:(part_idx + 1) * head_cols], w_output[part_idx * head_cols:(part_idx + 1) * head_cols], preferred_element_type=jnp.float32)
        partial_value = lax.optimization_barrier(partial_value.astype(jnp.bfloat16))
        total = total + partial_value.astype(jnp.float32)
    attend_out = total.astype(jnp.bfloat16)
    moe_normed = rms_scale(x_experts, expert_gain).reshape(N_EP, TOK_M, D)
    route_blocks = routes.reshape(N_EP, TOK_M, TOPK)
    dest_slot, slot_tok = jax.vmap(slot_plan)(route_blocks)
    padded_rows = jnp.concatenate([moe_normed, jnp.zeros((N_EP, 1, D), jnp.bfloat16)], axis=1)
    outgoing = jax.vmap(lambda rows_all, index_all: rows_all[index_all])(padded_rows, slot_tok)
    inbound = outgoing.reshape(N_EP, EXPERTS, CAP, D).transpose(1, 0, 2, 3)
    unit_cols = FF // N_TP

    def one_expert(operands):
        rows_in, gate_mat, up_mat, down_mat = operands
        flat_rows = rows_in.reshape(N_EP * CAP, D)
        gate_act = jnp.dot(flat_rows, gate_mat, preferred_element_type=jnp.float32)
        up_act = jnp.dot(flat_rows, up_mat, preferred_element_type=jnp.float32)
        hidden = (jax.nn.silu(gate_act) * up_act).astype(jnp.bfloat16)
        summed = jnp.zeros((N_EP * CAP, D), jnp.float32)
        for part_idx in range(N_TP):
            partial_value = jnp.dot(hidden[:, part_idx * unit_cols:(part_idx + 1) * unit_cols], down_mat[part_idx * unit_cols:(part_idx + 1) * unit_cols], preferred_element_type=jnp.float32)
            partial_value = lax.optimization_barrier(partial_value.astype(jnp.bfloat16))
            summed = summed + partial_value.astype(jnp.float32)
        return summed.astype(jnp.bfloat16).reshape(N_EP, CAP, D)
    results = lax.map(one_expert, (inbound, w_gate, w_up, w_down))
    back_rows = results.transpose(1, 0, 2, 3).reshape(N_EP, EXPERTS * CAP, D)
    picked = jax.vmap(lambda rows_all, index_all: rows_all[index_all])(back_rows, dest_slot).astype(jnp.float32)
    route_weight = group_prob[:, None] * expert_prob / lax.optimization_barrier(jnp.sum(expert_prob, axis=1, keepdims=True))
    expert_out = lax.optimization_barrier(jnp.sum(picked.reshape(TOKENS_M, TOPK, D) * route_weight[:, :, None], axis=1)).astype(jnp.bfloat16)
    return (attend_out, expert_out)
```

```python
import functools

import jax
import jax.numpy as jnp
from jax import lax
from jax.experimental import pallas as pl
from jax.experimental.pallas import tpu as pltpu
from jax.sharding import PartitionSpec as P

HEAD_DIM = 64
WINDOW = 128
GRID_W = 64
MESH = pl.DeviceIdType.MESH


epsilon = 1e-06
rope_base = 10000.0


def extended(x, sides, width):
    for axis, dim in sides:
        peers, length = (lax.axis_size(axis), x.shape[dim])
        up = [(i, (i + 1) % peers) for i in range(peers - 1)]
        down = [(j, i) for i, j in up]
        last = lax.slice_in_dim(x, length - width, length, axis=dim)
        initial = lax.slice_in_dim(x, 0, width, axis=dim)
        before = lax.ppermute(last, axis, up)
        after = lax.ppermute(initial, axis, down)
        x = jnp.concatenate([before, x, after], axis=dim)
    return x


def rms_scale(inputs, gain):
    values_f = inputs.astype(jnp.float32)
    scaled = values_f * lax.rsqrt(jnp.mean(values_f * values_f, axis=-1, keepdims=True) + epsilon)
    return (scaled * gain).astype(jnp.bfloat16)


def rope_tables(positions):
    grid_rows = (positions // GRID_W).astype(jnp.float32)
    grid_cols = (positions % GRID_W).astype(jnp.float32)
    half_dim = HEAD_DIM // 2
    inverse = rope_base ** (-jnp.arange(0, half_dim, 2, dtype=jnp.float32) / half_dim)
    angles = jnp.concatenate([grid_rows[:, None] * inverse, grid_cols[:, None] * inverse], axis=-1)
    return (jnp.cos(angles), jnp.sin(angles))


def head_norm_rope(projected, gain, cosine, sine_tab):
    scaled = (
        projected
        * lax.rsqrt(jnp.mean(projected * projected, axis=-1, keepdims=True) + epsilon)
        * gain
    )
    first_half, second_half = jnp.split(scaled, 2, axis=-1)
    cos_b = cosine[:, None, :]
    sin_b = sine_tab[:, None, :]
    turned = jnp.concatenate(
        [first_half * cos_b - second_half * sin_b, second_half * cos_b + first_half * sin_b],
        axis=-1,
    )
    return turned.astype(jnp.bfloat16)


def flip(a, b, count):
    total, bit = 0, 1
    while bit < count:
        total = total + lax.rem(a // bit + b // bit, 2) * bit
        bit *= 2
    return total


def exchange_kernel(
    n_ep,
    send_ref,
    gate_ref,
    up_ref,
    down_ref,
    mix_ref,
    attn_ref,
    out_ref,
    attn_out_ref,
    rows_buf,
    part_out,
    part_keep,
    part_in,
    y_out,
    y_own,
    y_in,
    final,
    back,
    total,
    attn_in,
    attn_y_out,
    attn_y_in,
    local_sem,
    d_send, d_recv,
    p_send, p_recv,
    y_send, y_recv,
    r_send, r_recv,
    c_send, c_recv,
    s_send, s_recv,
    f_send, f_recv,
    a_send, a_recv,
):
    me = lax.axis_index("ep")
    lane = lax.axis_index("tp")
    core = lax.rem(lane, 2)
    side = lane // 2
    other_core, other_side = 1 - core, 1 - side
    partner = 2 * side + other_core
    across = 2 * other_side + core
    width = send_ref.shape[2]

    barrier = pltpu.get_barrier_semaphore()

    def greet(k, carry):
        pl.semaphore_signal(
            barrier, inc=1, device_id={"ep": flip(me, k, n_ep), "tp": lane}, device_id_type=MESH
        )
        return carry

    lax.fori_loop(1, n_ep, greet, 0)
    for peer in (partner, across):
        pl.semaphore_signal(barrier, inc=1, device_id={"ep": me, "tp": peer}, device_id_type=MESH)
    pl.semaphore_wait(barrier, n_ep + 1)

    def remote(src, dst, sends, recvs, k, ep, tp):
        return pltpu.make_async_remote_copy(
            src_ref=src,
            dst_ref=dst,
            send_sem=sends.at[k],
            recv_sem=recvs.at[k],
            device_id={"ep": ep, "tp": tp},
            device_id_type=MESH,
        )

    def dispatch(k):
        dest = flip(me, k, n_ep)
        return remote(send_ref.at[dest], rows_buf.at[lane, k], d_send, d_recv, k, dest, lane)

    def to_partner(k):
        block = rows_buf.at[lane, k]
        return remote(block, block, p_send, p_recv, k, me, partner)

    def to_across(k):
        block = rows_buf.at[lane, k]
        return remote(block, block, y_send, y_recv, k, me, across)

    def relay(k):
        block = rows_buf.at[across, k]
        return remote(block, block, r_send, r_recv, k, me, partner)

    def sum_core(k):
        return remote(part_out.at[k], part_in.at[k], c_send, c_recv, k, me, partner)

    def sum_side(k):
        return remote(y_out.at[k], y_in.at[k], s_send, s_recv, k, me, across)

    def give_back(k):
        return remote(final.at[k], back.at[k], f_send, f_recv, k, flip(me, k, n_ep), lane)

    def attn_core(s):
        return remote(
            attn_ref.at[2 * s + other_core], attn_in.at[s], a_send, a_recv, s, me, partner
        )

    def attn_side():
        return remote(attn_y_out, attn_y_in, a_send, a_recv, 2, me, across)

    own = pltpu.make_async_copy(send_ref.at[me], rows_buf.at[lane, 0], local_sem)
    own.start()

    def start_dispatch(k, carry):
        dispatch(k).start()
        return carry

    lax.fori_loop(1, n_ep, start_dispatch, 0)
    attn_core(0).start()
    attn_core(1).start()
    total[...] = jnp.zeros_like(total)
    own.wait()

    def step(t, carry):
        @pl.when(t < n_ep)
        def _():
            @pl.when(t > 0)
            def _():
                dispatch(t).wait_recv()

            to_partner(t).start()
            to_across(t).start()

        k5 = t - 3

        @pl.when((k5 >= 0) & (k5 < n_ep))
        def _():
            sum_core(k5).wait_recv()
            y_out[k5] = (
                part_keep[k5, other_side].astype(jnp.float32)
                + part_in[k5, other_side].astype(jnp.float32)
            ).astype(jnp.bfloat16)
            sum_side(k5).start()
            y_own[k5] = part_keep[k5, side].astype(jnp.float32) + part_in[k5, side].astype(
                jnp.float32
            )

        k1 = t - 1

        @pl.when((k1 >= 0) & (k1 < n_ep))
        def _():
            to_across(k1).wait_recv()
            relay(k1).start()

        k2 = t - 2

        @pl.when((k2 >= 0) & (k2 < n_ep))
        def _():
            to_partner(k2).wait_recv()
            relay(k2).wait_recv()
            gate = jnp.zeros((send_ref.shape[1], gate_ref.shape[1]), jnp.float32)
            up = gate
            for q in range(4):
                rows = rows_buf[q, k2]
                span = slice(q * width, (q + 1) * width)
                gate += jnp.dot(rows, gate_ref[span, :], preferred_element_type=jnp.float32)
                up += jnp.dot(rows, up_ref[span, :], preferred_element_type=jnp.float32)
            hidden = (gate / (1.0 + jnp.exp(-gate)) * up).astype(jnp.bfloat16)
            for s in range(2):
                for c, target in ((other_core, part_out), (core, part_keep)):
                    start = pl.multiple_of((2 * s + c) * width, width)
                    target[k2, s] = jnp.dot(
                        hidden, down_ref[:, pl.ds(start, width)], preferred_element_type=jnp.float32
                    ).astype(jnp.bfloat16)
            sum_core(k2).start()

        k6 = t - 4

        @pl.when((k6 >= 0) & (k6 < n_ep))
        def _():
            sum_side(k6).wait_recv()
            final[k6] = (y_own[k6] + y_in[k6].astype(jnp.float32)).astype(jnp.bfloat16)

            @pl.when(k6 > 0)
            def _():
                give_back(k6).start()

            @pl.when(k6 == 0)
            def _():
                total[...] += jnp.dot(mix_ref[me], final[0], preferred_element_type=jnp.float32)

        k7 = t - 6

        @pl.when((k7 > 0) & (k7 < n_ep))
        def _():
            give_back(k7).wait_recv()
            total[...] += jnp.dot(
                mix_ref[flip(me, k7, n_ep)], back[k7], preferred_element_type=jnp.float32
            )

        @pl.when(t == 1)
        def _():
            attn_core(0).wait_recv()
            attn_core(1).wait_recv()
            attn_y_out[...] = (
                attn_ref[2 * other_side + core].astype(jnp.float32)
                + attn_in[other_side].astype(jnp.float32)
            ).astype(jnp.bfloat16)
            attn_side().start()

        return carry

    lax.fori_loop(0, n_ep + 6, step, 0)
    attn_side().wait_recv()
    attn_out_ref[...] = (
        attn_ref[2 * side + core].astype(jnp.float32)
        + attn_in[side].astype(jnp.float32)
        + attn_y_in[...].astype(jnp.float32)
    ).astype(jnp.bfloat16)
    out_ref[...] = total[...].astype(jnp.bfloat16)

    def drain(k, carry):
        @pl.when(k > 0)
        def _():
            dispatch(k).wait_send()
            give_back(k).wait_send()

        to_partner(k).wait_send()
        to_across(k).wait_send()
        relay(k).wait_send()
        sum_core(k).wait_send()
        sum_side(k).wait_send()
        return carry

    lax.fori_loop(0, n_ep, drain, 0)
    attn_core(0).wait_send()
    attn_core(1).wait_send()
    attn_side().wait_send()


def per_device(
    x_attend,
    attend_gain,
    w_query,
    w_key,
    w_value,
    query_gain,
    key_gain,
    sink_logit,
    w_output,
    x_experts,
    expert_gain,
    routes,
    group_prob,
    expert_prob,
    w_gate,
    w_up,
    w_down,
):
    tok_rows = x_attend.shape[0]
    model_width = x_attend.shape[1]
    heads_local = sink_logit.shape[0]
    kv_local = w_key.shape[1] // HEAD_DIM
    group = heads_local // kv_local
    offset = lax.axis_index("ep") * tok_rows
    positions = offset + jnp.arange(tok_rows, dtype=jnp.int32)
    cosine, sine_tab = rope_tables(positions)
    normed = rms_scale(x_attend, attend_gain)
    queries = head_norm_rope(
        jnp.dot(normed, w_query, preferred_element_type=jnp.float32).reshape(
            tok_rows, heads_local, HEAD_DIM
        ),
        query_gain,
        cosine,
        sine_tab,
    )
    key_rows = head_norm_rope(
        jnp.dot(normed, w_key, preferred_element_type=jnp.float32).reshape(
            tok_rows, kv_local, HEAD_DIM
        ),
        key_gain,
        cosine,
        sine_tab,
    )
    values = jnp.dot(normed, w_value, preferred_element_type=jnp.float32).astype(jnp.bfloat16)
    stacked = jnp.stack([key_rows.reshape(tok_rows, kv_local * HEAD_DIM), values], axis=0)
    padded = extended(stacked, (("ep", 1),), WINDOW)
    span_keys = padded[0].reshape(tok_rows + 2 * WINDOW, kv_local, HEAD_DIM)
    span_values = padded[1].reshape(tok_rows + 2 * WINDOW, kv_local, HEAD_DIM)
    scores = jnp.einsum(
        "qhgd,khd->hgqk",
        queries.reshape(tok_rows, kv_local, group, HEAD_DIM),
        span_keys,
        preferred_element_type=jnp.float32,
    ) * HEAD_DIM ** (-0.5)
    key_pos = offset - WINDOW + jnp.arange(tok_rows + 2 * WINDOW, dtype=jnp.int32)
    total_len = tok_rows * lax.axis_size("ep")
    in_window = (
        (jnp.abs(positions[:, None] - key_pos[None, :]) <= WINDOW)
        & (key_pos[None, :] >= 0)
        & (key_pos[None, :] < total_len)
    )
    scores = jnp.where(in_window[None, None], scores, -1e30)
    sink_col = sink_logit.reshape(kv_local, group)[:, :, None]
    peak = jnp.maximum(jnp.max(scores, axis=-1), sink_col)[..., None]
    weights = jnp.exp(scores - peak)
    denominator = jnp.sum(weights, axis=-1, keepdims=True) + jnp.exp(sink_col[..., None] - peak)
    probs = (weights / denominator).astype(jnp.bfloat16)
    attended = jnp.einsum("hgqk,khd->qhgd", probs, span_values, preferred_element_type=jnp.float32)
    attended = attended.astype(jnp.bfloat16).reshape(tok_rows, heads_local * HEAD_DIM)
    tp_count = lax.axis_size("tp")
    attn_part = (
        jnp.dot(attended, w_output, preferred_element_type=jnp.float32)
        .astype(jnp.bfloat16)
        .reshape(tp_count, tok_rows // tp_count, model_width)
    )
    moe_rows = x_experts.shape[0]
    top_count = routes.shape[1]
    n_ep = lax.axis_size("ep")
    capacity = max(2, (3 * moe_rows * top_count + 2 * n_ep - 1) // (2 * n_ep))
    moe_normed = rms_scale(x_experts, expert_gain)
    col_width = model_width // tp_count
    own_cols = lax.dynamic_slice_in_dim(moe_normed, lax.axis_index("tp") * col_width, col_width, 1)
    route_weight = group_prob[:, None] * expert_prob / jnp.sum(expert_prob, axis=1, keepdims=True)
    names = jnp.arange(n_ep, dtype=jnp.int32)
    chosen = routes[:, :, None] == names[None, None, :]
    named = jnp.any(chosen, axis=1)
    token = jnp.arange(moe_rows, dtype=jnp.int32)
    earlier = (token[None, :] < token[:, None]).astype(jnp.bfloat16)
    rank = jnp.dot(earlier, named.astype(jnp.bfloat16), preferred_element_type=jnp.float32)
    rank = jnp.where(named, rank.astype(jnp.int32), -1)
    share = jnp.sum(jnp.where(chosen, route_weight[:, :, None], 0.0), axis=1)
    slots = jnp.arange(capacity, dtype=jnp.int32)
    pick = (rank.T[:, None, :] == slots[None, :, None]).astype(jnp.bfloat16)
    outgoing = jnp.dot(
        pick.reshape(n_ep * capacity, moe_rows), own_cols, preferred_element_type=jnp.float32
    )
    outgoing = outgoing.astype(jnp.bfloat16).reshape(n_ep, capacity, col_width)
    mix = jnp.where(
        rank.T[:, :, None] == slots[None, None, :], share.T[:, :, None], 0.0
    ).astype(jnp.bfloat16)
    hidden_cols = w_gate.shape[2]
    slice_rows = tok_rows // tp_count
    bf16, f32 = jnp.bfloat16, jnp.float32
    vmem = pl.BlockSpec(memory_space=pltpu.VMEM)
    dma = pltpu.SemaphoreType.DMA
    expert_out, attend_out = pl.pallas_call(
        functools.partial(exchange_kernel, n_ep),
        out_shape=(
            jax.ShapeDtypeStruct((moe_rows, col_width), bf16),
            jax.ShapeDtypeStruct((slice_rows, model_width), bf16),
        ),
        in_specs=[vmem] * 6,
        out_specs=(vmem, vmem),
        scratch_shapes=[
            pltpu.VMEM((tp_count, n_ep, capacity, col_width), bf16),
            pltpu.VMEM((n_ep, 2, capacity, col_width), bf16),
            pltpu.VMEM((n_ep, 2, capacity, col_width), bf16),
            pltpu.VMEM((n_ep, 2, capacity, col_width), bf16),
            pltpu.VMEM((n_ep, capacity, col_width), bf16),
            pltpu.VMEM((n_ep, capacity, col_width), f32),
            pltpu.VMEM((n_ep, capacity, col_width), bf16),
            pltpu.VMEM((n_ep, capacity, col_width), bf16),
            pltpu.VMEM((n_ep, capacity, col_width), bf16),
            pltpu.VMEM((moe_rows, col_width), f32),
            pltpu.VMEM((2, slice_rows, model_width), bf16),
            pltpu.VMEM((slice_rows, model_width), bf16),
            pltpu.VMEM((slice_rows, model_width), bf16),
            dma(()),
        ]
        + [dma((n_ep,))] * 14
        + [dma((3,))] * 2,
        compiler_params=pltpu.CompilerParams(
            collective_id=0, has_side_effects=True, vmem_limit_bytes=60 * 1024 * 1024
        ),
    )(outgoing, w_gate[0], w_up[0], w_down[0], mix, attn_part)
    return (attend_out, expert_out)


def solution(mesh):
    placed = (
        P("ep", None),
        P(),
        P(None, "tp"),
        P(None, "tp"),
        P(None, "tp"),
        P(),
        P(),
        P("tp"),
        P("tp", None),
        P("ep", None),
        P(),
        P("ep", None),
        P("ep"),
        P("ep", None),
        P("ep", None, "tp"),
        P("ep", None, "tp"),
        P("ep", "tp", None),
    )
    return jax.shard_map(
        per_device,
        mesh=mesh,
        in_specs=placed,
        out_specs=(P(("ep", "tp"), None), P("ep", "tp")),
        check_vma=False,
    )
```

```python
import functools

import jax
import jax.numpy as jnp
from jax import lax
from jax.experimental import pallas as pl
from jax.experimental.pallas import tpu as pltpu
from jax.sharding import PartitionSpec as P

HEAD_DIM = 64
WINDOW = 128
GRID_W = 64
MESH = pl.DeviceIdType.MESH


epsilon = 1e-06
rope_base = 10000.0


def extended(x, sides, width):
    for axis, dim in sides:
        peers, length = (lax.axis_size(axis), x.shape[dim])
        up = [(i, (i + 1) % peers) for i in range(peers - 1)]
        down = [(j, i) for i, j in up]
        last = lax.slice_in_dim(x, length - width, length, axis=dim)
        initial = lax.slice_in_dim(x, 0, width, axis=dim)
        before = lax.ppermute(last, axis, up)
        after = lax.ppermute(initial, axis, down)
        x = jnp.concatenate([before, x, after], axis=dim)
    return x


def rms_scale(inputs, gain):
    values_f = inputs.astype(jnp.float32)
    scaled = values_f * lax.rsqrt(jnp.mean(values_f * values_f, axis=-1, keepdims=True) + epsilon)
    return (scaled * gain).astype(jnp.bfloat16)


def rope_tables(positions):
    grid_rows = (positions // GRID_W).astype(jnp.float32)
    grid_cols = (positions % GRID_W).astype(jnp.float32)
    half_dim = HEAD_DIM // 2
    inverse = rope_base ** (-jnp.arange(0, half_dim, 2, dtype=jnp.float32) / half_dim)
    angles = jnp.concatenate([grid_rows[:, None] * inverse, grid_cols[:, None] * inverse], axis=-1)
    return (jnp.cos(angles), jnp.sin(angles))


def head_norm_rope(projected, gain, cosine, sine_tab):
    scaled = (
        projected
        * lax.rsqrt(jnp.mean(projected * projected, axis=-1, keepdims=True) + epsilon)
        * gain
    )
    first_half, second_half = jnp.split(scaled, 2, axis=-1)
    cos_b = cosine[:, None, :]
    sin_b = sine_tab[:, None, :]
    turned = jnp.concatenate(
        [first_half * cos_b - second_half * sin_b, second_half * cos_b + first_half * sin_b],
        axis=-1,
    )
    return turned.astype(jnp.bfloat16)


def flip(a, b, count):
    total, bit = 0, 1
    while bit < count:
        total = total + lax.rem(a // bit + b // bit, 2) * bit
        bit *= 2
    return total


def turn(p, count):
    half = count // 2
    return jnp.where(p == 0, 0, jnp.where(p <= half, p + half - 1, p - half))


def exchange_kernel(
    n_ep,
    pick_ref,
    normed_ref,
    gate_ref,
    up_ref,
    down_ref,
    mix_ref,
    attn_ref,
    out_ref,
    attn_out_ref,
    send_own,
    send_other,
    rows_buf,
    part_out,
    part_keep,
    part_in,
    y_out,
    y_own,
    y_in,
    final,
    back,
    total,
    attn_in,
    attn_y_out,
    attn_y_in,
    d_send, d_recv,
    e_send, e_recv,
    p_send, p_recv,
    y_send, y_recv,
    r_send, r_recv,
    c_send, c_recv,
    s_send, s_recv,
    f_send, f_recv,
    a_send, a_recv,
):
    me = lax.axis_index("ep")
    lane = lax.axis_index("tp")
    core = lax.rem(lane, 2)
    side = lane // 2
    other_core, other_side = 1 - core, 1 - side
    partner = 2 * side + other_core
    across = 2 * other_side + core
    capacity, width = send_own.shape[1:]
    half = n_ep // 2

    barrier = pltpu.get_barrier_semaphore()

    def greet(k, carry):
        pl.semaphore_signal(
            barrier, inc=1, device_id={"ep": flip(me, k, n_ep), "tp": lane}, device_id_type=MESH
        )
        return carry

    lax.fori_loop(1, n_ep, greet, 0)
    for peer in (partner, across):
        pl.semaphore_signal(barrier, inc=1, device_id={"ep": me, "tp": peer}, device_id_type=MESH)
    pl.semaphore_wait(barrier, n_ep + 1)

    def remote(src, dst, sends, recvs, k, ep, tp):
        return pltpu.make_async_remote_copy(
            src_ref=src,
            dst_ref=dst,
            send_sem=sends.at[k],
            recv_sem=recvs.at[k],
            device_id={"ep": ep, "tp": tp},
            device_id_type=MESH,
        )

    def dispatch(k):
        dest = flip(me, k, n_ep)
        return remote(send_own.at[k], rows_buf.at[lane, k], d_send, d_recv, k, dest, lane)

    def dispatch_other(k):
        dest = flip(me, k, n_ep)
        return remote(send_other.at[k], rows_buf.at[across, k], e_send, e_recv, k, dest, lane)

    def to_partner(k):
        block = rows_buf.at[lane, k]
        return remote(block, block, p_send, p_recv, k, me, partner)

    def to_across(k):
        block = rows_buf.at[lane, k]
        return remote(block, block, y_send, y_recv, k, me, across)

    def relay(k):
        block = rows_buf.at[across, k]
        return remote(block, block, r_send, r_recv, k, me, partner)

    def sum_core(k):
        return remote(part_out.at[k], part_in.at[k], c_send, c_recv, k, me, partner)

    def sum_side(k):
        return remote(y_out.at[k], y_in.at[k], s_send, s_recv, k, me, across)

    def give_back(k):
        return remote(final.at[k], back.at[k], f_send, f_recv, k, flip(me, k, n_ep), lane)

    def attn_core(s):
        return remote(
            attn_ref.at[2 * s + other_core], attn_in.at[s], a_send, a_recv, s, me, partner
        )

    def attn_side():
        return remote(attn_y_out, attn_y_in, a_send, a_recv, 2, me, across)

    def gathered(k, quarter):
        start = pl.multiple_of(quarter * width, width)
        rows = jnp.dot(
            pick_ref[flip(me, k, n_ep)],
            normed_ref[:, pl.ds(start, width)],
            preferred_element_type=jnp.float32,
        )
        return rows.astype(jnp.bfloat16)

    def start_dispatch(p, carry):
        k = turn(p, n_ep)
        send_own[k] = gathered(k, lane)
        dispatch(k).start()

        @pl.when(k < half)
        def _():
            send_other[k] = gathered(k, across)
            dispatch_other(k).start()

        return carry

    lax.fori_loop(1, n_ep, start_dispatch, 0)
    rows_buf[lane, 0] = gathered(0, lane)
    rows_buf[across, 0] = gathered(0, across)
    attn_core(0).start()
    attn_core(1).start()
    total[...] = jnp.zeros_like(total)

    def step(t, carry):
        @pl.when(t < n_ep)
        def _():
            k0 = turn(t, n_ep)

            @pl.when(k0 > 0)
            def _():
                dispatch(k0).wait_recv()

            to_partner(k0).start()

            @pl.when(k0 >= half)
            def _():
                to_across(k0).start()

            @pl.when((k0 > 0) & (k0 < half))
            def _():
                dispatch_other(k0).wait_recv()

            @pl.when(k0 < half)
            def _():
                relay(k0).start()

        p5 = t - 3

        @pl.when((p5 >= 0) & (p5 < n_ep))
        def _():
            k5 = turn(p5, n_ep)
            sum_core(k5).wait_recv()
            y_out[k5] = (
                part_keep[k5, other_side].astype(jnp.float32)
                + part_in[k5, other_side].astype(jnp.float32)
            ).astype(jnp.bfloat16)
            sum_side(k5).start()
            y_own[k5] = part_keep[k5, side].astype(jnp.float32) + part_in[k5, side].astype(
                jnp.float32
            )

        p1 = t - 1

        @pl.when((p1 >= 0) & (p1 < n_ep))
        def _():
            k1 = turn(p1, n_ep)

            @pl.when(k1 >= half)
            def _():
                to_across(k1).wait_recv()
                relay(k1).start()

        p2 = t - 2

        @pl.when((p2 >= 0) & (p2 < n_ep))
        def _():
            k2 = turn(p2, n_ep)
            to_partner(k2).wait_recv()
            relay(k2).wait_recv()
            gate = jnp.zeros((capacity, gate_ref.shape[1]), jnp.float32)
            up = gate
            for q in range(4):
                rows = rows_buf[q, k2]
                span = slice(q * width, (q + 1) * width)
                gate += jnp.dot(rows, gate_ref[span, :], preferred_element_type=jnp.float32)
                up += jnp.dot(rows, up_ref[span, :], preferred_element_type=jnp.float32)
            hidden = (gate / (1.0 + jnp.exp(-gate)) * up).astype(jnp.bfloat16)
            for s in range(2):
                for c, target in ((other_core, part_out), (core, part_keep)):
                    start = pl.multiple_of((2 * s + c) * width, width)
                    target[k2, s] = jnp.dot(
                        hidden, down_ref[:, pl.ds(start, width)], preferred_element_type=jnp.float32
                    ).astype(jnp.bfloat16)
            sum_core(k2).start()

        p6 = t - 4

        @pl.when((p6 >= 0) & (p6 < n_ep))
        def _():
            k6 = turn(p6, n_ep)
            sum_side(k6).wait_recv()
            final[k6] = (y_own[k6] + y_in[k6].astype(jnp.float32)).astype(jnp.bfloat16)

            @pl.when(k6 > 0)
            def _():
                give_back(k6).start()

            @pl.when(k6 == 0)
            def _():
                total[...] += jnp.dot(mix_ref[me], final[0], preferred_element_type=jnp.float32)

        p7 = t - 6

        @pl.when((p7 > 0) & (p7 < n_ep))
        def _():
            k7 = turn(p7, n_ep)
            give_back(k7).wait_recv()
            total[...] += jnp.dot(
                mix_ref[flip(me, k7, n_ep)], back[k7], preferred_element_type=jnp.float32
            )

        @pl.when(t == n_ep)
        def _():
            attn_core(0).wait_recv()
            attn_core(1).wait_recv()
            attn_y_out[...] = (
                attn_ref[2 * other_side + core].astype(jnp.float32)
                + attn_in[other_side].astype(jnp.float32)
            ).astype(jnp.bfloat16)
            attn_side().start()

        return carry

    lax.fori_loop(0, n_ep + 6, step, 0)
    attn_side().wait_recv()
    attn_out_ref[...] = (
        attn_ref[2 * side + core].astype(jnp.float32)
        + attn_in[side].astype(jnp.float32)
        + attn_y_in[...].astype(jnp.float32)
    ).astype(jnp.bfloat16)
    out_ref[...] = total[...].astype(jnp.bfloat16)

    def drain(k, carry):
        @pl.when(k > 0)
        def _():
            dispatch(k).wait_send()
            give_back(k).wait_send()

        to_partner(k).wait_send()
        @pl.when(k >= half)
        def _():
            to_across(k).wait_send()

        @pl.when((k > 0) & (k < half))
        def _():
            dispatch_other(k).wait_send()

        relay(k).wait_send()
        sum_core(k).wait_send()
        sum_side(k).wait_send()
        return carry

    lax.fori_loop(0, n_ep, drain, 0)
    attn_core(0).wait_send()
    attn_core(1).wait_send()
    attn_side().wait_send()


def per_device(
    x_attend,
    attend_gain,
    w_query,
    w_key,
    w_value,
    query_gain,
    key_gain,
    sink_logit,
    w_output,
    x_experts,
    expert_gain,
    routes,
    group_prob,
    expert_prob,
    w_gate,
    w_up,
    w_down,
):
    tok_rows = x_attend.shape[0]
    model_width = x_attend.shape[1]
    heads_local = sink_logit.shape[0]
    kv_local = w_key.shape[1] // HEAD_DIM
    group = heads_local // kv_local
    offset = lax.axis_index("ep") * tok_rows
    positions = offset + jnp.arange(tok_rows, dtype=jnp.int32)
    cosine, sine_tab = rope_tables(positions)
    normed = rms_scale(x_attend, attend_gain)
    queries = head_norm_rope(
        jnp.dot(normed, w_query, preferred_element_type=jnp.float32).reshape(
            tok_rows, heads_local, HEAD_DIM
        ),
        query_gain,
        cosine,
        sine_tab,
    )
    key_rows = head_norm_rope(
        jnp.dot(normed, w_key, preferred_element_type=jnp.float32).reshape(
            tok_rows, kv_local, HEAD_DIM
        ),
        key_gain,
        cosine,
        sine_tab,
    )
    values = jnp.dot(normed, w_value, preferred_element_type=jnp.float32).astype(jnp.bfloat16)
    stacked = jnp.stack([key_rows.reshape(tok_rows, kv_local * HEAD_DIM), values], axis=0)
    padded = extended(stacked, (("ep", 1),), WINDOW)
    span_keys = padded[0].reshape(tok_rows + 2 * WINDOW, kv_local, HEAD_DIM)
    span_values = padded[1].reshape(tok_rows + 2 * WINDOW, kv_local, HEAD_DIM)
    scores = jnp.einsum(
        "qhgd,khd->hgqk",
        queries.reshape(tok_rows, kv_local, group, HEAD_DIM),
        span_keys,
        preferred_element_type=jnp.float32,
    ) * HEAD_DIM ** (-0.5)
    key_pos = offset - WINDOW + jnp.arange(tok_rows + 2 * WINDOW, dtype=jnp.int32)
    total_len = tok_rows * lax.axis_size("ep")
    in_window = (
        (jnp.abs(positions[:, None] - key_pos[None, :]) <= WINDOW)
        & (key_pos[None, :] >= 0)
        & (key_pos[None, :] < total_len)
    )
    scores = jnp.where(in_window[None, None], scores, -1e30)
    sink_col = sink_logit.reshape(kv_local, group)[:, :, None]
    peak = jnp.maximum(jnp.max(scores, axis=-1), sink_col)[..., None]
    weights = jnp.exp(scores - peak)
    denominator = jnp.sum(weights, axis=-1, keepdims=True) + jnp.exp(sink_col[..., None] - peak)
    probs = (weights / denominator).astype(jnp.bfloat16)
    attended = jnp.einsum("hgqk,khd->qhgd", probs, span_values, preferred_element_type=jnp.float32)
    attended = attended.astype(jnp.bfloat16).reshape(tok_rows, heads_local * HEAD_DIM)
    tp_count = lax.axis_size("tp")
    attn_part = (
        jnp.dot(attended, w_output, preferred_element_type=jnp.float32)
        .astype(jnp.bfloat16)
        .reshape(tp_count, tok_rows // tp_count, model_width)
    )
    moe_rows = x_experts.shape[0]
    top_count = routes.shape[1]
    n_ep = lax.axis_size("ep")
    capacity = max(2, (3 * moe_rows * top_count + 2 * n_ep - 1) // (2 * n_ep))
    moe_normed = rms_scale(x_experts, expert_gain)
    col_width = model_width // tp_count
    route_weight = group_prob[:, None] * expert_prob / jnp.sum(expert_prob, axis=1, keepdims=True)
    names = jnp.arange(n_ep, dtype=jnp.int32)
    chosen = routes[:, :, None] == names[None, None, :]
    named = jnp.any(chosen, axis=1)
    token = jnp.arange(moe_rows, dtype=jnp.int32)
    earlier = (token[None, :] < token[:, None]).astype(jnp.bfloat16)
    rank = jnp.dot(earlier, named.astype(jnp.bfloat16), preferred_element_type=jnp.float32)
    rank = jnp.where(named, rank.astype(jnp.int32), -1)
    share = jnp.sum(jnp.where(chosen, route_weight[:, :, None], 0.0), axis=1)
    slots = jnp.arange(capacity, dtype=jnp.int32)
    pick = (rank.T[:, None, :] == slots[None, :, None]).astype(jnp.bfloat16)
    mix = jnp.where(
        rank.T[:, :, None] == slots[None, None, :], share.T[:, :, None], 0.0
    ).astype(jnp.bfloat16)
    hidden_cols = w_gate.shape[2]
    slice_rows = tok_rows // tp_count
    bf16, f32 = jnp.bfloat16, jnp.float32
    vmem = pl.BlockSpec(memory_space=pltpu.VMEM)
    dma = pltpu.SemaphoreType.DMA
    expert_out, attend_out = pl.pallas_call(
        functools.partial(exchange_kernel, n_ep),
        out_shape=(
            jax.ShapeDtypeStruct((moe_rows, col_width), bf16),
            jax.ShapeDtypeStruct((slice_rows, model_width), bf16),
        ),
        in_specs=[vmem] * 7,
        out_specs=(vmem, vmem),
        scratch_shapes=[
            pltpu.VMEM((n_ep, capacity, col_width), bf16),
            pltpu.VMEM((n_ep // 2, capacity, col_width), bf16),
            pltpu.VMEM((tp_count, n_ep, capacity, col_width), bf16),
            pltpu.VMEM((n_ep, 2, capacity, col_width), bf16),
            pltpu.VMEM((n_ep, 2, capacity, col_width), bf16),
            pltpu.VMEM((n_ep, 2, capacity, col_width), bf16),
            pltpu.VMEM((n_ep, capacity, col_width), bf16),
            pltpu.VMEM((n_ep, capacity, col_width), f32),
            pltpu.VMEM((n_ep, capacity, col_width), bf16),
            pltpu.VMEM((n_ep, capacity, col_width), bf16),
            pltpu.VMEM((n_ep, capacity, col_width), bf16),
            pltpu.VMEM((moe_rows, col_width), f32),
            pltpu.VMEM((2, slice_rows, model_width), bf16),
            pltpu.VMEM((slice_rows, model_width), bf16),
            pltpu.VMEM((slice_rows, model_width), bf16),
        ]
        + [dma((n_ep,))] * 16
        + [dma((3,))] * 2,
        compiler_params=pltpu.CompilerParams(
            collective_id=0, has_side_effects=True, vmem_limit_bytes=60 * 1024 * 1024
        ),
    )(pick, moe_normed, w_gate[0], w_up[0], w_down[0], mix, attn_part)
    return (attend_out, expert_out)


def solution(mesh):
    placed = (
        P("ep", None),
        P(),
        P(None, "tp"),
        P(None, "tp"),
        P(None, "tp"),
        P(),
        P(),
        P("tp"),
        P("tp", None),
        P("ep", None),
        P(),
        P("ep", None),
        P("ep"),
        P("ep", None),
        P("ep", None, "tp"),
        P("ep", None, "tp"),
        P("ep", "tp", None),
    )
    return jax.shard_map(
        per_device,
        mesh=mesh,
        in_specs=placed,
        out_specs=(P(("ep", "tp"), None), P("ep", "tp")),
        check_vma=False,
    )
```

```python
import functools

import jax
import jax.numpy as jnp
from jax import lax
from jax.experimental import pallas as pl
from jax.experimental.pallas import tpu as pltpu
from jax.sharding import PartitionSpec as P

HEAD_DIM = 64
WINDOW = 128
GRID_W = 64
MESH = pl.DeviceIdType.MESH


epsilon = 1e-06
rope_base = 10000.0


def extended(x, sides, width):
    for axis, dim in sides:
        peers, length = (lax.axis_size(axis), x.shape[dim])
        up = [(i, (i + 1) % peers) for i in range(peers - 1)]
        down = [(j, i) for i, j in up]
        last = lax.slice_in_dim(x, length - width, length, axis=dim)
        initial = lax.slice_in_dim(x, 0, width, axis=dim)
        before = lax.ppermute(last, axis, up)
        after = lax.ppermute(initial, axis, down)
        x = jnp.concatenate([before, x, after], axis=dim)
    return x


def rms_scale(inputs, gain):
    values_f = inputs.astype(jnp.float32)
    scaled = values_f * lax.rsqrt(jnp.mean(values_f * values_f, axis=-1, keepdims=True) + epsilon)
    return (scaled * gain).astype(jnp.bfloat16)


def rope_tables(positions):
    grid_rows = (positions // GRID_W).astype(jnp.float32)
    grid_cols = (positions % GRID_W).astype(jnp.float32)
    half_dim = HEAD_DIM // 2
    inverse = rope_base ** (-jnp.arange(0, half_dim, 2, dtype=jnp.float32) / half_dim)
    angles = jnp.concatenate([grid_rows[:, None] * inverse, grid_cols[:, None] * inverse], axis=-1)
    return (jnp.cos(angles), jnp.sin(angles))


def head_norm_rope(projected, gain, cosine, sine_tab):
    scaled = (
        projected
        * lax.rsqrt(jnp.mean(projected * projected, axis=-1, keepdims=True) + epsilon)
        * gain
    )
    first_half, second_half = jnp.split(scaled, 2, axis=-1)
    cos_b = cosine[:, None, :]
    sin_b = sine_tab[:, None, :]
    turned = jnp.concatenate(
        [first_half * cos_b - second_half * sin_b, second_half * cos_b + first_half * sin_b],
        axis=-1,
    )
    return turned.astype(jnp.bfloat16)


def flip(a, b, count):
    total, bit = 0, 1
    while bit < count:
        total = total + lax.rem(a // bit + b // bit, 2) * bit
        bit *= 2
    return total


def turn(p, count):
    half = count // 2
    return jnp.where(p == 0, 0, jnp.where(p <= half, p + half - 1, p - half))


def exchange_kernel(
    n_ep,
    pick_ref,
    normed_ref,
    gate_ref,
    up_ref,
    down_ref,
    mix_ref,
    attn_ref,
    out_ref,
    attn_out_ref,
    send_own,
    send_other,
    rows_buf,
    part_out,
    part_keep,
    part_in,
    y_out,
    y_own,
    y_in,
    final,
    back,
    total,
    attn_in,
    attn_y_out,
    attn_y_in,
    d_send, d_recv,
    e_send, e_recv,
    p_send, p_recv,
    y_send, y_recv,
    r_send, r_recv,
    c_send, c_recv,
    s_send, s_recv,
    f_send, f_recv,
    a_send, a_recv,
):
    me = lax.axis_index("ep")
    lane = lax.axis_index("tp")
    core = lax.rem(lane, 2)
    side = lane // 2
    other_core, other_side = 1 - core, 1 - side
    partner = 2 * side + other_core
    across = 2 * other_side + core
    capacity, width = send_own.shape[1:]
    half = n_ep // 2

    barrier = pltpu.get_barrier_semaphore()

    def greet(k, carry):
        pl.semaphore_signal(
            barrier, inc=1, device_id={"ep": flip(me, k, n_ep), "tp": lane}, device_id_type=MESH
        )
        return carry

    lax.fori_loop(1, n_ep, greet, 0)
    for peer in (partner, across):
        pl.semaphore_signal(barrier, inc=1, device_id={"ep": me, "tp": peer}, device_id_type=MESH)
    pl.semaphore_wait(barrier, n_ep + 1)

    def remote(src, dst, sends, recvs, k, ep, tp):
        return pltpu.make_async_remote_copy(
            src_ref=src,
            dst_ref=dst,
            send_sem=sends.at[k],
            recv_sem=recvs.at[k],
            device_id={"ep": ep, "tp": tp},
            device_id_type=MESH,
        )

    def dispatch(k):
        dest = flip(me, k, n_ep)
        return remote(send_own.at[k], rows_buf.at[lane, k], d_send, d_recv, k, dest, lane)

    def dispatch_other(k):
        dest = flip(me, k, n_ep)
        return remote(send_other.at[k], rows_buf.at[across, k], e_send, e_recv, k, dest, lane)

    def to_partner(k):
        block = rows_buf.at[lane, k]
        return remote(block, block, p_send, p_recv, k, me, partner)

    def to_across(k):
        block = rows_buf.at[lane, k]
        return remote(block, block, y_send, y_recv, k, me, across)

    def relay(k):
        block = rows_buf.at[across, k]
        return remote(block, block, r_send, r_recv, k, me, partner)

    def sum_core(k):
        return remote(part_out.at[k], part_in.at[k], c_send, c_recv, k, me, partner)

    def sum_side(k):
        return remote(y_out.at[k], y_in.at[k], s_send, s_recv, k, me, across)

    def give_back(k):
        return remote(final.at[k], back.at[k], f_send, f_recv, k, flip(me, k, n_ep), lane)

    def attn_core(s):
        return remote(
            attn_ref.at[2 * s + other_core], attn_in.at[s], a_send, a_recv, s, me, partner
        )

    def attn_side():
        return remote(attn_y_out, attn_y_in, a_send, a_recv, 2, me, across)

    def gathered(k, quarter):
        start = pl.multiple_of(quarter * width, width)
        rows = jnp.dot(
            pick_ref[flip(me, k, n_ep)],
            normed_ref[:, pl.ds(start, width)],
            preferred_element_type=jnp.float32,
        )
        return rows.astype(jnp.bfloat16)

    def start_dispatch(p, carry):
        k = turn(p, n_ep)
        send_own[k] = gathered(k, lane)
        dispatch(k).start()

        @pl.when(k < half)
        def _():
            send_other[k] = gathered(k, across)
            dispatch_other(k).start()

        return carry

    lax.fori_loop(1, n_ep, start_dispatch, 0)
    rows_buf[lane, 0] = gathered(0, lane)
    rows_buf[across, 0] = gathered(0, across)
    attn_core(0).start()
    attn_core(1).start()
    total[...] = jnp.zeros_like(total)

    def step(t, carry):
        @pl.when(t < n_ep)
        def _():
            k0 = turn(t, n_ep)

            @pl.when(k0 > 0)
            def _():
                dispatch(k0).wait_recv()

            to_partner(k0).start()

            @pl.when(k0 >= half)
            def _():
                to_across(k0).start()

            @pl.when((k0 > 0) & (k0 < half))
            def _():
                dispatch_other(k0).wait_recv()

            @pl.when(k0 < half)
            def _():
                relay(k0).start()

        p5 = t - 4

        @pl.when((p5 >= 0) & (p5 < n_ep))
        def _():
            k5 = turn(p5, n_ep)
            sum_core(k5).wait_recv()
            y_out[k5] = (
                part_keep[k5, other_side].astype(jnp.float32)
                + part_in[k5, other_side].astype(jnp.float32)
            ).astype(jnp.bfloat16)
            sum_side(k5).start()
            y_own[k5] = part_keep[k5, side].astype(jnp.float32) + part_in[k5, side].astype(
                jnp.float32
            )

        p1 = t - 2

        @pl.when((p1 >= 0) & (p1 < n_ep))
        def _():
            k1 = turn(p1, n_ep)

            @pl.when(k1 >= half)
            def _():
                to_across(k1).wait_recv()
                relay(k1).start()

        p2 = t - 3

        @pl.when((p2 >= 0) & (p2 < n_ep))
        def _():
            k2 = turn(p2, n_ep)
            to_partner(k2).wait_recv()
            relay(k2).wait_recv()
            gate = jnp.zeros((capacity, gate_ref.shape[1]), jnp.float32)
            up = gate
            for q in range(4):
                rows = rows_buf[q, k2]
                span = slice(q * width, (q + 1) * width)
                gate += jnp.dot(rows, gate_ref[span, :], preferred_element_type=jnp.float32)
                up += jnp.dot(rows, up_ref[span, :], preferred_element_type=jnp.float32)
            hidden = (gate / (1.0 + jnp.exp(-gate)) * up).astype(jnp.bfloat16)
            for s in range(2):
                for c, target in ((other_core, part_out), (core, part_keep)):
                    start = pl.multiple_of((2 * s + c) * width, width)
                    target[k2, s] = jnp.dot(
                        hidden, down_ref[:, pl.ds(start, width)], preferred_element_type=jnp.float32
                    ).astype(jnp.bfloat16)
            sum_core(k2).start()

        p6 = t - 6

        @pl.when((p6 >= 0) & (p6 < n_ep))
        def _():
            k6 = turn(p6, n_ep)
            sum_side(k6).wait_recv()
            final[k6] = (y_own[k6] + y_in[k6].astype(jnp.float32)).astype(jnp.bfloat16)

            @pl.when(k6 > 0)
            def _():
                give_back(k6).start()

            @pl.when(k6 == 0)
            def _():
                total[...] += jnp.dot(mix_ref[me], final[0], preferred_element_type=jnp.float32)

        p7 = t - 9

        @pl.when((p7 > 0) & (p7 < n_ep))
        def _():
            k7 = turn(p7, n_ep)
            give_back(k7).wait_recv()
            total[...] += jnp.dot(
                mix_ref[flip(me, k7, n_ep)], back[k7], preferred_element_type=jnp.float32
            )

        @pl.when(t == 0)
        def _():
            attn_core(0).wait_recv()
            attn_core(1).wait_recv()
            attn_y_out[...] = (
                attn_ref[2 * other_side + core].astype(jnp.float32)
                + attn_in[other_side].astype(jnp.float32)
            ).astype(jnp.bfloat16)
            attn_side().start()

        return carry

    lax.fori_loop(0, n_ep + 9, step, 0)
    attn_side().wait_recv()
    attn_out_ref[...] = (
        attn_ref[2 * side + core].astype(jnp.float32)
        + attn_in[side].astype(jnp.float32)
        + attn_y_in[...].astype(jnp.float32)
    ).astype(jnp.bfloat16)
    out_ref[...] = total[...].astype(jnp.bfloat16)

    def drain(k, carry):
        @pl.when(k > 0)
        def _():
            dispatch(k).wait_send()
            give_back(k).wait_send()

        to_partner(k).wait_send()
        @pl.when(k >= half)
        def _():
            to_across(k).wait_send()

        @pl.when((k > 0) & (k < half))
        def _():
            dispatch_other(k).wait_send()

        relay(k).wait_send()
        sum_core(k).wait_send()
        sum_side(k).wait_send()
        return carry

    lax.fori_loop(0, n_ep, drain, 0)
    attn_core(0).wait_send()
    attn_core(1).wait_send()
    attn_side().wait_send()


def per_device(
    x_attend,
    attend_gain,
    w_query,
    w_key,
    w_value,
    query_gain,
    key_gain,
    sink_logit,
    w_output,
    x_experts,
    expert_gain,
    routes,
    group_prob,
    expert_prob,
    w_gate,
    w_up,
    w_down,
):
    tok_rows = x_attend.shape[0]
    model_width = x_attend.shape[1]
    heads_local = sink_logit.shape[0]
    kv_local = w_key.shape[1] // HEAD_DIM
    group = heads_local // kv_local
    offset = lax.axis_index("ep") * tok_rows
    positions = offset + jnp.arange(tok_rows, dtype=jnp.int32)
    cosine, sine_tab = rope_tables(positions)
    normed = rms_scale(x_attend, attend_gain)
    queries = head_norm_rope(
        jnp.dot(normed, w_query, preferred_element_type=jnp.float32).reshape(
            tok_rows, heads_local, HEAD_DIM
        ),
        query_gain,
        cosine,
        sine_tab,
    )
    key_rows = head_norm_rope(
        jnp.dot(normed, w_key, preferred_element_type=jnp.float32).reshape(
            tok_rows, kv_local, HEAD_DIM
        ),
        key_gain,
        cosine,
        sine_tab,
    )
    values = jnp.dot(normed, w_value, preferred_element_type=jnp.float32).astype(jnp.bfloat16)
    stacked = jnp.stack([key_rows.reshape(tok_rows, kv_local * HEAD_DIM), values], axis=0)
    padded = extended(stacked, (("ep", 1),), WINDOW)
    span_keys = padded[0].reshape(tok_rows + 2 * WINDOW, kv_local, HEAD_DIM)
    span_values = padded[1].reshape(tok_rows + 2 * WINDOW, kv_local, HEAD_DIM)
    scores = jnp.einsum(
        "qhgd,khd->hgqk",
        queries.reshape(tok_rows, kv_local, group, HEAD_DIM),
        span_keys,
        preferred_element_type=jnp.float32,
    ) * HEAD_DIM ** (-0.5)
    key_pos = offset - WINDOW + jnp.arange(tok_rows + 2 * WINDOW, dtype=jnp.int32)
    total_len = tok_rows * lax.axis_size("ep")
    in_window = (
        (jnp.abs(positions[:, None] - key_pos[None, :]) <= WINDOW)
        & (key_pos[None, :] >= 0)
        & (key_pos[None, :] < total_len)
    )
    scores = jnp.where(in_window[None, None], scores, -1e30)
    sink_col = sink_logit.reshape(kv_local, group)[:, :, None]
    peak = jnp.maximum(jnp.max(scores, axis=-1), sink_col)[..., None]
    weights = jnp.exp(scores - peak)
    denominator = jnp.sum(weights, axis=-1, keepdims=True) + jnp.exp(sink_col[..., None] - peak)
    probs = (weights / denominator).astype(jnp.bfloat16)
    attended = jnp.einsum("hgqk,khd->qhgd", probs, span_values, preferred_element_type=jnp.float32)
    attended = attended.astype(jnp.bfloat16).reshape(tok_rows, heads_local * HEAD_DIM)
    tp_count = lax.axis_size("tp")
    attn_part = (
        jnp.dot(attended, w_output, preferred_element_type=jnp.float32)
        .astype(jnp.bfloat16)
        .reshape(tp_count, tok_rows // tp_count, model_width)
    )
    moe_rows = x_experts.shape[0]
    top_count = routes.shape[1]
    n_ep = lax.axis_size("ep")
    capacity = max(2, (3 * moe_rows * top_count + 2 * n_ep - 1) // (2 * n_ep))
    moe_normed = rms_scale(x_experts, expert_gain)
    col_width = model_width // tp_count
    route_weight = group_prob[:, None] * expert_prob / jnp.sum(expert_prob, axis=1, keepdims=True)
    names = jnp.arange(n_ep, dtype=jnp.int32)
    chosen = routes[:, :, None] == names[None, None, :]
    named = jnp.any(chosen, axis=1)
    token = jnp.arange(moe_rows, dtype=jnp.int32)
    earlier = (token[None, :] < token[:, None]).astype(jnp.bfloat16)
    rank = jnp.dot(earlier, named.astype(jnp.bfloat16), preferred_element_type=jnp.float32)
    rank = jnp.where(named, rank.astype(jnp.int32), -1)
    share = jnp.sum(jnp.where(chosen, route_weight[:, :, None], 0.0), axis=1)
    slots = jnp.arange(capacity, dtype=jnp.int32)
    pick = (rank.T[:, None, :] == slots[None, :, None]).astype(jnp.bfloat16)
    mix = jnp.where(
        rank.T[:, :, None] == slots[None, None, :], share.T[:, :, None], 0.0
    ).astype(jnp.bfloat16)
    hidden_cols = w_gate.shape[2]
    slice_rows = tok_rows // tp_count
    bf16, f32 = jnp.bfloat16, jnp.float32
    vmem = pl.BlockSpec(memory_space=pltpu.VMEM)
    dma = pltpu.SemaphoreType.DMA
    expert_out, attend_out = pl.pallas_call(
        functools.partial(exchange_kernel, n_ep),
        out_shape=(
            jax.ShapeDtypeStruct((moe_rows, col_width), bf16),
            jax.ShapeDtypeStruct((slice_rows, model_width), bf16),
        ),
        in_specs=[vmem] * 7,
        out_specs=(vmem, vmem),
        scratch_shapes=[
            pltpu.VMEM((n_ep, capacity, col_width), bf16),
            pltpu.VMEM((n_ep // 2, capacity, col_width), bf16),
            pltpu.VMEM((tp_count, n_ep, capacity, col_width), bf16),
            pltpu.VMEM((n_ep, 2, capacity, col_width), bf16),
            pltpu.VMEM((n_ep, 2, capacity, col_width), bf16),
            pltpu.VMEM((n_ep, 2, capacity, col_width), bf16),
            pltpu.VMEM((n_ep, capacity, col_width), bf16),
            pltpu.VMEM((n_ep, capacity, col_width), f32),
            pltpu.VMEM((n_ep, capacity, col_width), bf16),
            pltpu.VMEM((n_ep, capacity, col_width), bf16),
            pltpu.VMEM((n_ep, capacity, col_width), bf16),
            pltpu.VMEM((moe_rows, col_width), f32),
            pltpu.VMEM((2, slice_rows, model_width), bf16),
            pltpu.VMEM((slice_rows, model_width), bf16),
            pltpu.VMEM((slice_rows, model_width), bf16),
        ]
        + [dma((n_ep,))] * 16
        + [dma((3,))] * 2,
        compiler_params=pltpu.CompilerParams(
            collective_id=0, has_side_effects=True, vmem_limit_bytes=60 * 1024 * 1024
        ),
    )(pick, moe_normed, w_gate[0], w_up[0], w_down[0], mix, attn_part)
    return (attend_out, expert_out)


def solution(mesh):
    placed = (
        P("ep", None),
        P(),
        P(None, "tp"),
        P(None, "tp"),
        P(None, "tp"),
        P(),
        P(),
        P("tp"),
        P("tp", None),
        P("ep", None),
        P(),
        P("ep", None),
        P("ep"),
        P("ep", None),
        P("ep", None, "tp"),
        P("ep", None, "tp"),
        P("ep", "tp", None),
    )
    return jax.shard_map(
        per_device,
        mesh=mesh,
        in_specs=placed,
        out_specs=(P(("ep", "tp"), None), P("ep", "tp")),
        check_vma=False,
    )
```

```python
import functools

import jax
import jax.numpy as jnp
from jax import lax
from jax.experimental import pallas as pl
from jax.experimental.pallas import tpu as pltpu
from jax.sharding import PartitionSpec as P

HEAD_DIM = 64
WINDOW = 128
GRID_W = 64
MESH = pl.DeviceIdType.MESH


epsilon = 1e-06
rope_base = 10000.0


def extended(x, sides, width):
    for axis, dim in sides:
        peers, length = (lax.axis_size(axis), x.shape[dim])
        up = [(i, (i + 1) % peers) for i in range(peers - 1)]
        down = [(j, i) for i, j in up]
        last = lax.slice_in_dim(x, length - width, length, axis=dim)
        initial = lax.slice_in_dim(x, 0, width, axis=dim)
        before = lax.ppermute(last, axis, up)
        after = lax.ppermute(initial, axis, down)
        x = jnp.concatenate([before, x, after], axis=dim)
    return x


def rms_scale(inputs, gain):
    values_f = inputs.astype(jnp.float32)
    scaled = values_f * lax.rsqrt(jnp.mean(values_f * values_f, axis=-1, keepdims=True) + epsilon)
    return (scaled * gain).astype(jnp.bfloat16)


def rope_tables(positions):
    grid_rows = (positions // GRID_W).astype(jnp.float32)
    grid_cols = (positions % GRID_W).astype(jnp.float32)
    half_dim = HEAD_DIM // 2
    inverse = rope_base ** (-jnp.arange(0, half_dim, 2, dtype=jnp.float32) / half_dim)
    angles = jnp.concatenate([grid_rows[:, None] * inverse, grid_cols[:, None] * inverse], axis=-1)
    return (jnp.cos(angles), jnp.sin(angles))


def head_norm_rope(projected, gain, cosine, sine_tab):
    scaled = (
        projected
        * lax.rsqrt(jnp.mean(projected * projected, axis=-1, keepdims=True) + epsilon)
        * gain
    )
    first_half, second_half = jnp.split(scaled, 2, axis=-1)
    cos_b = cosine[:, None, :]
    sin_b = sine_tab[:, None, :]
    turned = jnp.concatenate(
        [first_half * cos_b - second_half * sin_b, second_half * cos_b + first_half * sin_b],
        axis=-1,
    )
    return turned.astype(jnp.bfloat16)


def flip(a, b, count):
    total, bit = 0, 1
    while bit < count:
        total = total + lax.rem(a // bit + b // bit, 2) * bit
        bit *= 2
    return total


def turn(p, count):
    return p // 2 + lax.rem(p, 2) * (count // 2)


def exchange_kernel(
    n_ep,
    pick_ref,
    normed_ref,
    gate_ref,
    up_ref,
    down_ref,
    mix_ref,
    attn_ref,
    out_ref,
    attn_out_ref,
    send_own,
    send_other,
    rows_buf,
    part_out,
    part_keep,
    part_in,
    y_out,
    y_own,
    y_in,
    final,
    back,
    total,
    attn_in,
    attn_y_out,
    attn_y_in,
    d_send, d_recv,
    e_send, e_recv,
    p_send, p_recv,
    y_send, y_recv,
    r_send, r_recv,
    c_send, c_recv,
    s_send, s_recv,
    f_send, f_recv,
    a_send, a_recv,
):
    me = lax.axis_index("ep")
    lane = lax.axis_index("tp")
    core = lax.rem(lane, 2)
    side = lane // 2
    other_core, other_side = 1 - core, 1 - side
    partner = 2 * side + other_core
    across = 2 * other_side + core
    capacity, width = send_own.shape[1:]
    half = n_ep // 2

    barrier = pltpu.get_barrier_semaphore()

    def greet(k, carry):
        pl.semaphore_signal(
            barrier, inc=1, device_id={"ep": flip(me, k, n_ep), "tp": lane}, device_id_type=MESH
        )
        return carry

    lax.fori_loop(1, n_ep, greet, 0)
    for peer in (partner, across):
        pl.semaphore_signal(barrier, inc=1, device_id={"ep": me, "tp": peer}, device_id_type=MESH)
    pl.semaphore_wait(barrier, n_ep + 1)

    def remote(src, dst, sends, recvs, k, ep, tp):
        return pltpu.make_async_remote_copy(
            src_ref=src,
            dst_ref=dst,
            send_sem=sends.at[k],
            recv_sem=recvs.at[k],
            device_id={"ep": ep, "tp": tp},
            device_id_type=MESH,
        )

    def dispatch(k):
        dest = flip(me, k, n_ep)
        return remote(send_own.at[k], rows_buf.at[lane, k], d_send, d_recv, k, dest, lane)

    def dispatch_other(k):
        dest = flip(me, k, n_ep)
        return remote(send_other.at[k], rows_buf.at[across, k], e_send, e_recv, k, dest, lane)

    def to_partner(k):
        block = rows_buf.at[lane, k]
        return remote(block, block, p_send, p_recv, k, me, partner)

    def to_across(k):
        block = rows_buf.at[lane, k]
        return remote(block, block, y_send, y_recv, k, me, across)

    def relay(k):
        block = rows_buf.at[across, k]
        return remote(block, block, r_send, r_recv, k, me, partner)

    def sum_core(k):
        return remote(part_out.at[k], part_in.at[k], c_send, c_recv, k, me, partner)

    def sum_side(k):
        return remote(y_out.at[k], y_in.at[k], s_send, s_recv, k, me, across)

    def give_back(k):
        return remote(final.at[k], back.at[k], f_send, f_recv, k, flip(me, k, n_ep), lane)

    def attn_core(s):
        return remote(
            attn_ref.at[2 * s + other_core], attn_in.at[s], a_send, a_recv, s, me, partner
        )

    def attn_side():
        return remote(attn_y_out, attn_y_in, a_send, a_recv, 2, me, across)

    def gathered(k, quarter):
        start = pl.multiple_of(quarter * width, width)
        rows = jnp.dot(
            pick_ref[flip(me, k, n_ep)],
            normed_ref[:, pl.ds(start, width)],
            preferred_element_type=jnp.float32,
        )
        return rows.astype(jnp.bfloat16)

    def start_dispatch(p, carry):
        k = turn(p, n_ep)
        send_own[k] = gathered(k, lane)
        dispatch(k).start()

        @pl.when(k < half)
        def _():
            send_other[k] = gathered(k, across)
            dispatch_other(k).start()

        return carry

    lax.fori_loop(1, n_ep, start_dispatch, 0)
    rows_buf[lane, 0] = gathered(0, lane)
    rows_buf[across, 0] = gathered(0, across)
    attn_core(0).start()
    attn_core(1).start()
    total[...] = jnp.zeros_like(total)

    def step(t, carry):
        @pl.when(t < n_ep)
        def _():
            k0 = turn(t, n_ep)

            @pl.when(k0 > 0)
            def _():
                dispatch(k0).wait_recv()

            to_partner(k0).start()

            @pl.when(k0 >= half)
            def _():
                to_across(k0).start()

            @pl.when((k0 > 0) & (k0 < half))
            def _():
                dispatch_other(k0).wait_recv()

            @pl.when(k0 < half)
            def _():
                relay(k0).start()

        p5 = t - 4

        @pl.when((p5 >= 0) & (p5 < n_ep))
        def _():
            k5 = turn(p5, n_ep)
            sum_core(k5).wait_recv()
            y_out[k5] = (
                part_keep[k5, other_side].astype(jnp.float32)
                + part_in[k5, other_side].astype(jnp.float32)
            ).astype(jnp.bfloat16)
            sum_side(k5).start()
            y_own[k5] = part_keep[k5, side].astype(jnp.float32) + part_in[k5, side].astype(
                jnp.float32
            )

        p1 = t - 2

        @pl.when((p1 >= 0) & (p1 < n_ep))
        def _():
            k1 = turn(p1, n_ep)

            @pl.when(k1 >= half)
            def _():
                to_across(k1).wait_recv()
                relay(k1).start()

        p2 = t - 3

        @pl.when((p2 >= 0) & (p2 < n_ep))
        def _():
            k2 = turn(p2, n_ep)
            to_partner(k2).wait_recv()
            relay(k2).wait_recv()
            gate = jnp.zeros((capacity, gate_ref.shape[1]), jnp.float32)
            up = gate
            for q in range(4):
                rows = rows_buf[q, k2]
                span = slice(q * width, (q + 1) * width)
                gate += jnp.dot(rows, gate_ref[span, :], preferred_element_type=jnp.float32)
                up += jnp.dot(rows, up_ref[span, :], preferred_element_type=jnp.float32)
            hidden = (gate / (1.0 + jnp.exp(-gate)) * up).astype(jnp.bfloat16)
            for s in range(2):
                for c, target in ((other_core, part_out), (core, part_keep)):
                    start = pl.multiple_of((2 * s + c) * width, width)
                    target[k2, s] = jnp.dot(
                        hidden, down_ref[:, pl.ds(start, width)], preferred_element_type=jnp.float32
                    ).astype(jnp.bfloat16)
            sum_core(k2).start()

        p6 = t - 6

        @pl.when((p6 >= 0) & (p6 < n_ep))
        def _():
            k6 = turn(p6, n_ep)
            sum_side(k6).wait_recv()
            final[k6] = (y_own[k6] + y_in[k6].astype(jnp.float32)).astype(jnp.bfloat16)

            @pl.when(k6 > 0)
            def _():
                give_back(k6).start()

            @pl.when(k6 == 0)
            def _():
                total[...] += jnp.dot(mix_ref[me], final[0], preferred_element_type=jnp.float32)

        p7 = t - 9

        @pl.when((p7 > 0) & (p7 < n_ep))
        def _():
            k7 = turn(p7, n_ep)
            give_back(k7).wait_recv()
            total[...] += jnp.dot(
                mix_ref[flip(me, k7, n_ep)], back[k7], preferred_element_type=jnp.float32
            )

        @pl.when(t == 0)
        def _():
            attn_core(0).wait_recv()
            attn_core(1).wait_recv()
            attn_y_out[...] = (
                attn_ref[2 * other_side + core].astype(jnp.float32)
                + attn_in[other_side].astype(jnp.float32)
            ).astype(jnp.bfloat16)
            attn_side().start()

        return carry

    lax.fori_loop(0, n_ep + 9, step, 0)
    attn_side().wait_recv()
    attn_out_ref[...] = (
        attn_ref[2 * side + core].astype(jnp.float32)
        + attn_in[side].astype(jnp.float32)
        + attn_y_in[...].astype(jnp.float32)
    ).astype(jnp.bfloat16)
    out_ref[...] = total[...].astype(jnp.bfloat16)

    def drain(k, carry):
        @pl.when(k > 0)
        def _():
            dispatch(k).wait_send()
            give_back(k).wait_send()

        to_partner(k).wait_send()
        @pl.when(k >= half)
        def _():
            to_across(k).wait_send()

        @pl.when((k > 0) & (k < half))
        def _():
            dispatch_other(k).wait_send()

        relay(k).wait_send()
        sum_core(k).wait_send()
        sum_side(k).wait_send()
        return carry

    lax.fori_loop(0, n_ep, drain, 0)
    attn_core(0).wait_send()
    attn_core(1).wait_send()
    attn_side().wait_send()


def per_device(
    x_attend,
    attend_gain,
    w_query,
    w_key,
    w_value,
    query_gain,
    key_gain,
    sink_logit,
    w_output,
    x_experts,
    expert_gain,
    routes,
    group_prob,
    expert_prob,
    w_gate,
    w_up,
    w_down,
):
    tok_rows = x_attend.shape[0]
    model_width = x_attend.shape[1]
    heads_local = sink_logit.shape[0]
    kv_local = w_key.shape[1] // HEAD_DIM
    group = heads_local // kv_local
    offset = lax.axis_index("ep") * tok_rows
    positions = offset + jnp.arange(tok_rows, dtype=jnp.int32)
    cosine, sine_tab = rope_tables(positions)
    normed = rms_scale(x_attend, attend_gain)
    queries = head_norm_rope(
        jnp.dot(normed, w_query, preferred_element_type=jnp.float32).reshape(
            tok_rows, heads_local, HEAD_DIM
        ),
        query_gain,
        cosine,
        sine_tab,
    )
    key_rows = head_norm_rope(
        jnp.dot(normed, w_key, preferred_element_type=jnp.float32).reshape(
            tok_rows, kv_local, HEAD_DIM
        ),
        key_gain,
        cosine,
        sine_tab,
    )
    values = jnp.dot(normed, w_value, preferred_element_type=jnp.float32).astype(jnp.bfloat16)
    stacked = jnp.stack([key_rows.reshape(tok_rows, kv_local * HEAD_DIM), values], axis=0)
    padded = extended(stacked, (("ep", 1),), WINDOW)
    span_keys = padded[0].reshape(tok_rows + 2 * WINDOW, kv_local, HEAD_DIM)
    span_values = padded[1].reshape(tok_rows + 2 * WINDOW, kv_local, HEAD_DIM)
    scores = jnp.einsum(
        "qhgd,khd->hgqk",
        queries.reshape(tok_rows, kv_local, group, HEAD_DIM),
        span_keys,
        preferred_element_type=jnp.float32,
    ) * HEAD_DIM ** (-0.5)
    key_pos = offset - WINDOW + jnp.arange(tok_rows + 2 * WINDOW, dtype=jnp.int32)
    total_len = tok_rows * lax.axis_size("ep")
    in_window = (
        (jnp.abs(positions[:, None] - key_pos[None, :]) <= WINDOW)
        & (key_pos[None, :] >= 0)
        & (key_pos[None, :] < total_len)
    )
    scores = jnp.where(in_window[None, None], scores, -1e30)
    sink_col = sink_logit.reshape(kv_local, group)[:, :, None]
    peak = jnp.maximum(jnp.max(scores, axis=-1), sink_col)[..., None]
    weights = jnp.exp(scores - peak)
    denominator = jnp.sum(weights, axis=-1, keepdims=True) + jnp.exp(sink_col[..., None] - peak)
    probs = (weights / denominator).astype(jnp.bfloat16)
    attended = jnp.einsum("hgqk,khd->qhgd", probs, span_values, preferred_element_type=jnp.float32)
    attended = attended.astype(jnp.bfloat16).reshape(tok_rows, heads_local * HEAD_DIM)
    tp_count = lax.axis_size("tp")
    attn_part = (
        jnp.dot(attended, w_output, preferred_element_type=jnp.float32)
        .astype(jnp.bfloat16)
        .reshape(tp_count, tok_rows // tp_count, model_width)
    )
    moe_rows = x_experts.shape[0]
    top_count = routes.shape[1]
    n_ep = lax.axis_size("ep")
    capacity = max(2, (3 * moe_rows * top_count + 2 * n_ep - 1) // (2 * n_ep))
    moe_normed = rms_scale(x_experts, expert_gain)
    col_width = model_width // tp_count
    route_weight = group_prob[:, None] * expert_prob / jnp.sum(expert_prob, axis=1, keepdims=True)
    names = jnp.arange(n_ep, dtype=jnp.int32)
    chosen = routes[:, :, None] == names[None, None, :]
    named = jnp.any(chosen, axis=1)
    token = jnp.arange(moe_rows, dtype=jnp.int32)
    earlier = (token[None, :] < token[:, None]).astype(jnp.bfloat16)
    rank = jnp.dot(earlier, named.astype(jnp.bfloat16), preferred_element_type=jnp.float32)
    rank = jnp.where(named, rank.astype(jnp.int32), -1)
    share = jnp.sum(jnp.where(chosen, route_weight[:, :, None], 0.0), axis=1)
    slots = jnp.arange(capacity, dtype=jnp.int32)
    pick = (rank.T[:, None, :] == slots[None, :, None]).astype(jnp.bfloat16)
    mix = jnp.where(
        rank.T[:, :, None] == slots[None, None, :], share.T[:, :, None], 0.0
    ).astype(jnp.bfloat16)
    hidden_cols = w_gate.shape[2]
    slice_rows = tok_rows // tp_count
    bf16, f32 = jnp.bfloat16, jnp.float32
    vmem = pl.BlockSpec(memory_space=pltpu.VMEM)
    dma = pltpu.SemaphoreType.DMA
    expert_out, attend_out = pl.pallas_call(
        functools.partial(exchange_kernel, n_ep),
        out_shape=(
            jax.ShapeDtypeStruct((moe_rows, col_width), bf16),
            jax.ShapeDtypeStruct((slice_rows, model_width), bf16),
        ),
        in_specs=[vmem] * 7,
        out_specs=(vmem, vmem),
        scratch_shapes=[
            pltpu.VMEM((n_ep, capacity, col_width), bf16),
            pltpu.VMEM((n_ep // 2, capacity, col_width), bf16),
            pltpu.VMEM((tp_count, n_ep, capacity, col_width), bf16),
            pltpu.VMEM((n_ep, 2, capacity, col_width), bf16),
            pltpu.VMEM((n_ep, 2, capacity, col_width), bf16),
            pltpu.VMEM((n_ep, 2, capacity, col_width), bf16),
            pltpu.VMEM((n_ep, capacity, col_width), bf16),
            pltpu.VMEM((n_ep, capacity, col_width), f32),
            pltpu.VMEM((n_ep, capacity, col_width), bf16),
            pltpu.VMEM((n_ep, capacity, col_width), bf16),
            pltpu.VMEM((n_ep, capacity, col_width), bf16),
            pltpu.VMEM((moe_rows, col_width), f32),
            pltpu.VMEM((2, slice_rows, model_width), bf16),
            pltpu.VMEM((slice_rows, model_width), bf16),
            pltpu.VMEM((slice_rows, model_width), bf16),
        ]
        + [dma((n_ep,))] * 16
        + [dma((3,))] * 2,
        compiler_params=pltpu.CompilerParams(
            collective_id=0, has_side_effects=True, vmem_limit_bytes=60 * 1024 * 1024
        ),
    )(pick, moe_normed, w_gate[0], w_up[0], w_down[0], mix, attn_part)
    return (attend_out, expert_out)


def solution(mesh):
    placed = (
        P("ep", None),
        P(),
        P(None, "tp"),
        P(None, "tp"),
        P(None, "tp"),
        P(),
        P(),
        P("tp"),
        P("tp", None),
        P("ep", None),
        P(),
        P("ep", None),
        P("ep"),
        P("ep", None),
        P("ep", None, "tp"),
        P("ep", None, "tp"),
        P("ep", "tp", None),
    )
    return jax.shard_map(
        per_device,
        mesh=mesh,
        in_specs=placed,
        out_specs=(P(("ep", "tp"), None), P("ep", "tp")),
        check_vma=False,
    )
```
